32 devices in a mesh: ep: 8 (over z, x), tp: 4 (over y, core).
Axes of the slice: x: 2, y: 2, z: 4, core: 2. Of those that a mesh axis runs over, the one named last changes fastest.
Arguments:
- tokens: bfloat16 [128, 4096], P('ep'), may hold values from -6 to 6
- norm_gain: float32 [4096], replicated, may hold values from 0.1 to 1.9
- query_weight: bfloat16 [4096, 2048], P('ep', 'tp'), may hold values from -0.09375 to 0.09375
- key_weight: bfloat16 [4096, 256], P('ep', 'tp'), may hold values from -0.09375 to 0.09375
- value_weight: bfloat16 [4096, 256], P('ep', 'tp'), may hold values from -0.09375 to 0.09375
- forget_weight: bfloat16 [4096, 32], P('ep', 'tp'), may hold values from -0.09375 to 0.09375
- forget_bias: float32 [32], P('tp'), may hold values from -1 to 2
- kv_cache: bfloat16 [128, 1024, 4, 128], P('ep', None, 'tp'), may hold values from -256 to 256, as said below
- log_gates: float32 [128, 1024, 32], P('ep', None, 'tp'), may hold values from -258 to 0
- lengths: int32 [128], P('ep'), may hold values from 128 to 1024, as said below
- out_weight: bfloat16 [2048, 4096], P('tp', 'ep'), may hold values from -0.125 to 0.125
- mix_gain: float32 [4096], replicated, may hold values from 0.1 to 1.9
- expert_gate: bfloat16 [8, 4096, 1024], P('ep', None, 'tp'), may hold values from -0.09375 to 0.09375
- expert_up: bfloat16 [8, 4096, 1024], P('ep', None, 'tp'), may hold values from -0.09375 to 0.09375
- expert_down: bfloat16 [8, 1024, 4096], P('ep', 'tp'), may hold values from -0.1875 to 0.1875
- routes: int32 [128, 4], P('ep'), may hold values from 0 to 7, all different within a row; in each aligned block of 16 rows (0 to 15, 16 to 31, ...) at most 16 rows name the same one
- route_weights: float32 [128, 4], P('ep'), may hold values from 0.2 to 1
- dense_gate: bfloat16 [4096, 4096], P(None, 'ep'), may hold values from -0.09375 to 0.09375
- dense_up: bfloat16 [4096, 4096], P(None, 'ep'), may hold values from -0.09375 to 0.09375
- dense_down: bfloat16 [4096, 4096], P('ep', 'tp'), may hold values from -0.09375 to 0.09375
- gate_vector: float32 [4096], replicated, may hold values from -0.09375 to 0.09375
Outputs:
- layer_out: bfloat16 [128, 4096], P('ep', 'tp')
The draws below stay inside these ranges and needn't reach their ends.
Inputs may be any that keep to these rules, and one draw needn't show every extreme that they name: `kv_cache`: keys and values of the cached positions. `lengths`: some sequence uses all 1024 cached positions in every draw. A sequence's 4 experts differ. Among the routes of the 16 sequences of one index of ep no expert appears more than 16 times, and in every draw some expert appears exactly 16 times there; every expert is chosen somewhere.
All inputs are finite; a program needn't handle non-finite values.
Results may differ from the reference program's by a relative error of at most 0.012.
The reference program's roundings to bfloat16 on the way count: a program that leaves them out, or rounds other values in their place, can miss the bound.
Values may be sent and summed in bfloat16 or wider, within the bound.
A program may use at most 128 MiB of HBM per device.

```python
import math
import jax
import jax.numpy as jnp
import numpy as np
from jax import lax

D = 4096
HEADS = 32
KV_HEADS = 4
HD = 64
FE = 1024
FS = 4096
TOPK = 4
SEQ_DEV = 16
CACHE_POSITIONS = 1024
SEQUENCE_TOTAL = 128
EXPERTS = 8
CAP = 16
N_EP = 8


def log_uniform(stream, shape, low, high):
    return jnp.exp(jax.random.uniform(stream, shape, jnp.float32, math.log(low), math.log(high)))


def draw_kv_cache(key, part):
    sequence_flows = jax.random.split(key, 2)
    key_shape = (SEQUENCE_TOTAL, CACHE_POSITIONS, KV_HEADS, HD)
    key_part = jnp.clip(jax.random.normal(sequence_flows[0], key_shape, jnp.float32), -6.0, 6.0)
    value_base = jnp.clip(jax.random.normal(sequence_flows[1], key_shape, jnp.float32), -6.0, 6.0)
    return jnp.concatenate([key_part, value_base], axis=-1).astype(jnp.bfloat16)


def draw_log_gates(key, part):
    sequence_flows = jax.random.split(key, 8)
    slow_share = 0.5
    slow = jax.random.uniform(sequence_flows[0], (HEADS,)) < slow_share
    slow_total = log_uniform(sequence_flows[1], (HEADS,), 0.1, 0.5)
    fast_rate = log_uniform(sequence_flows[2], (HEADS,), 1.0 / 100.0, 1.0 / 30.0)
    base_rate = jnp.where(slow, slow_total / CACHE_POSITIONS, fast_rate)
    seq_factor = log_uniform(sequence_flows[3], (SEQUENCE_TOTAL, 1, 1), 0.5, 2.0)
    block_factor = jnp.repeat(log_uniform(sequence_flows[4], (SEQUENCE_TOTAL, 16, 1), 0.5, 2.0), CACHE_POSITIONS // 16, axis=1)
    roughness = jax.random.uniform(sequence_flows[5], (SEQUENCE_TOTAL, CACHE_POSITIONS, HEADS), jnp.float32, 0.5, 1.5)
    spike_locations = jax.random.randint(sequence_flows[6], (SEQUENCE_TOTAL, 2), 0, CACHE_POSITIONS)
    current_position = jnp.arange(CACHE_POSITIONS)
    spiking = jnp.any(current_position[None, :, None] == spike_locations[:, None, :], axis=2)
    spike_length = jax.random.uniform(sequence_flows[7], (SEQUENCE_TOTAL, CACHE_POSITIONS, 1), jnp.float32, 0.22, 0.5)
    reduction_amount = base_rate[None, None, :] * seq_factor * block_factor * roughness
    reduction_amount = reduction_amount + jnp.where(spiking[:, :, None], spike_length, 0.0)
    return jnp.cumsum(-reduction_amount, axis=1)


def draw_lengths(key, part):
    sequence_flows = jax.random.split(key, 2)
    picked = jax.random.randint(sequence_flows[0], (SEQUENCE_TOTAL,), CACHE_POSITIONS // 8, CACHE_POSITIONS + 1)
    chosen = jax.random.randint(sequence_flows[1], (), 0, SEQUENCE_TOTAL)
    return jnp.where(jnp.arange(SEQUENCE_TOTAL) == chosen, CACHE_POSITIONS, picked).astype(jnp.int32)


def steps_of(rng, dims, cuts, smallest, high):
    loudness = 1.0
    for position, blocks in cuts:
        steps = jax.random.uniform(jax.random.fold_in(jax.random.fold_in(rng, 6), position), (blocks,), jnp.float32, smallest / len(cuts), high / len(cuts))
        loudness = loudness * jnp.repeat(jnp.exp(steps), dims[position] // blocks).reshape((-1,) + (1,) * (len(dims) - 1 - position))
    return loudness


def assign_block(rng, own, number, rows, count, top, most, skew):
    ranking = jax.random.permutation(rng, count)
    packed, ordinary = portions_of(count, rows * top, most, skew, True), portions_of(count, rows * top, most, skew, False)
    places = jnp.arange(count)

    def named(tallies, offset_by):
        used = int((tallies > 0).sum())
        fixed = max(1, used // 4)
        moved = fixed + (places - fixed + offset_by * (used - fixed)) % max(1, count - fixed)
        return jnp.zeros((count,), jnp.int32).at[ranking[jnp.where(places < fixed, places, moved)]].set(jnp.asarray(tallies, jnp.int32))

    tallies = jnp.where(number % 4 == 0, named(packed, number // 4), named(ordinary, number - number // 4 - 1))
    mixed = jax.random.permutation(jax.random.fold_in(own, 3), count)
    giver, taker = mixed[0:count // 2 * 2:2], mixed[1:count // 2 * 2:2]
    margin = jnp.minimum(tallies[giver] - 1, most - tallies[taker]) // 2
    margin = jnp.where((giver == ranking[0]) | (taker == ranking[0]) | (tallies[taker] == 0), 0, jnp.maximum(margin, 0))
    moved = jax.random.randint(jax.random.fold_in(own, 4), (count // 2,), 0, 1 << 20) % (margin + 1)
    tallies = tallies.at[giver].add(-moved).at[taker].add(moved)
    members = jnp.searchsorted(jnp.cumsum(tallies), jnp.arange(rows * top), side="right").astype(jnp.int32)
    table = members.reshape(top, rows).T
    table = table[jax.random.permutation(jax.random.fold_in(own, 1), rows)]
    offset_by = jax.random.randint(jax.random.fold_in(own, 2), (rows, 1), 0, top)
    return jnp.take_along_axis(table, (jnp.arange(top)[None, :] + offset_by) % top, axis=1)


def portions_of(amount, total, reach, lean, full):
    weights = [(1 << 20) // math.isqrt(grade ** lean) + 1 for grade in range(1, amount + 1)]
    largest = reach if full else min(reach, max(-(-total // amount), total * weights[0] // sum(weights)))
    least = 1 if total - largest >= amount - 1 else 0
    holding, surplus = [largest] + [least] * (amount - 1), total - largest - least * (amount - 1)
    while surplus > 0:
        movable = [i for i in range(1, amount) if holding[i] < largest] or [i for i in range(1, amount) if holding[i] < reach]
        pool, left = sum([weights[i] for i in movable]), surplus
        for i in movable:
            addition = min(reach - holding[i], max(1, left * weights[i] // pool), surplus)
            holding[i] = holding[i] + addition
            surplus = surplus - addition
    return np.array(holding)


def gaussian(stream_key, dims, spread, limit, pieces=(), kind=jnp.bfloat16):
    values = jax.random.normal(stream_key, dims, jnp.float32) * spread
    if len(pieces) > 0:
        values = steps_of(stream_key, dims, pieces, -0.22, 0.18) * values
    return jnp.clip(values, min=-limit, max=limit).astype(kind)


def setup_inputs(seed: int = 0) -> dict:
    arg_keys = jax.random.split(jax.random.key(seed), 22)
    tokens = gaussian(arg_keys[0], (SEQUENCE_TOTAL, D), 1.0, 6.0, ((0, 8),))
    norm_gain = jnp.clip(1.0 + 0.18 * jax.random.normal(arg_keys[1], (D,), jnp.float32), 0.1, 1.9)
    query_weight = gaussian(arg_keys[2], (D, HEADS * HD), D ** -0.5, 0.09375, ((0, 8), (1, 4)))
    key_weight = gaussian(arg_keys[3], (D, KV_HEADS * HD), D ** -0.5, 0.09375, ((0, 8), (1, 4)))
    value_weight = gaussian(arg_keys[4], (D, KV_HEADS * HD), D ** -0.5, 0.09375, ((0, 8), (1, 4)))
    forget_weight = gaussian(arg_keys[5], (D, HEADS), D ** -0.5, 0.09375, ((0, 8), (1, 4)))
    forget_bias = jnp.clip(-1.0 + 3.0 * jax.random.uniform(arg_keys[6], (HEADS,), jnp.float32) ** steps_of(arg_keys[6], (HEADS,), ((0, 4),), -0.2, 0.2), -1.0, 2.0)
    kv_cache = draw_kv_cache(jax.random.fold_in(arg_keys[21], 71), 0)
    log_gates = draw_log_gates(jax.random.fold_in(arg_keys[21], 71), 0)
    lengths = draw_lengths(jax.random.fold_in(arg_keys[21], 71), 0)
    out_weight = gaussian(arg_keys[10], (HEADS * HD, D), (HEADS * HD) ** -0.5, 0.125, ((0, 4), (1, 8)))
    mix_gain = jnp.clip(1.0 + 0.18 * jax.random.normal(arg_keys[11], (D,), jnp.float32), 0.1, 1.9)
    expert_gate = gaussian(arg_keys[12], (EXPERTS, D, FE), D ** -0.5, 0.09375, ((0, 8), (2, 4)))
    expert_up = gaussian(arg_keys[13], (EXPERTS, D, FE), D ** -0.5, 0.09375, ((0, 8), (2, 4)))
    expert_down = gaussian(arg_keys[14], (EXPERTS, FE, D), FE ** -0.5, 0.1875, ((0, 8), (1, 4)))
    routes_keys = jax.random.split(jax.random.fold_in(arg_keys[15], 1), SEQUENCE_TOTAL // SEQ_DEV)
    routes_turns = jax.random.permutation(jax.random.fold_in(arg_keys[15], 3), SEQUENCE_TOTAL // SEQ_DEV)
    routes = jax.vmap(lambda own, number: assign_block(jax.random.fold_in(arg_keys[15], 2), own, number, SEQ_DEV, EXPERTS, TOPK, CAP, 2))(routes_keys, routes_turns).reshape((SEQUENCE_TOTAL, TOPK))
    route_weights = jnp.clip(0.2 + 0.8 * jax.random.uniform(arg_keys[16], (SEQUENCE_TOTAL, TOPK), jnp.float32) ** steps_of(arg_keys[16], (SEQUENCE_TOTAL, TOPK), ((0, 8),), -0.2, 0.2), 0.2, 1.0)
    dense_gate = gaussian(arg_keys[17], (D, FS), D ** -0.5, 0.09375, ((1, 8),))
    dense_up = gaussian(arg_keys[18], (D, FS), D ** -0.5, 0.09375, ((1, 8),))
    dense_down = gaussian(arg_keys[19], (FS, D), FS ** -0.5, 0.09375, ((0, 8), (1, 4)))
    gate_vector = gaussian(arg_keys[20], (D,), D ** -0.5, 0.09375, (), jnp.float32)
    return {"tokens": tokens, "norm_gain": norm_gain, "query_weight": query_weight, "key_weight": key_weight, "value_weight": value_weight, "forget_weight": forget_weight, "forget_bias": forget_bias, "kv_cache": kv_cache, "log_gates": log_gates, "lengths": lengths, "out_weight": out_weight, "mix_gain": mix_gain, "expert_gate": expert_gate, "expert_up": expert_up, "expert_down": expert_down, "routes": routes, "route_weights": route_weights, "dense_gate": dense_gate, "dense_up": dense_up, "dense_down": dense_down, "gate_vector": gate_vector}


EPS = 1e-06

def rms_scaled(matrix, gains):
    values = matrix.astype(jnp.float32)
    return values * lax.rsqrt(lax.optimization_barrier(jnp.mean(values * values, axis=-1, keepdims=True)) + EPS) * gains.astype(jnp.float32)

def attend_block(inputs):
    queries, key_new, value_new, forget, cache_rows, cum_gates, length = inputs
    seqs_here, cache_len = (cache_rows.shape[0], cache_rows.shape[1])
    kv_count, group_size, head_width = (queries.shape[1], queries.shape[2], queries.shape[3])
    cached_keys = cache_rows[..., :head_width].astype(jnp.float32)
    cached_values = cache_rows[..., head_width:].astype(jnp.float32)
    query_wide = queries.astype(jnp.float32)
    score_scale = head_width ** (-0.5)
    current_position = jnp.arange(cache_len, dtype=jnp.int32)
    is_last = (current_position[None, :] == length[:, None] - 1)[:, :, None]
    last_gate = lax.optimization_barrier(jnp.sum(jnp.where(is_last, cum_gates, 0.0), axis=1))
    newest = last_gate + forget
    gate_bias = newest[:, None, :] - cum_gates
    gate_bias = gate_bias.reshape(seqs_here, cache_len, kv_count, group_size).transpose(0, 2, 3, 1)
    past_scores = jnp.einsum('skgd,slkd->skgl', query_wide, cached_keys) * score_scale + gate_bias
    is_valid = (current_position[None, :] < length[:, None])[:, None, None, :]
    past_scores = jnp.where(is_valid, past_scores, -jnp.inf)
    own_score = jnp.einsum('skgd,skd->skg', query_wide, key_new.astype(jnp.float32)) * score_scale
    highest = jnp.maximum(lax.optimization_barrier(jnp.max(past_scores, axis=-1)), own_score)
    past_exp = jnp.exp(past_scores - highest[..., None])
    own_exp = jnp.exp(own_score - highest)
    totals = lax.optimization_barrier(jnp.sum(past_exp, axis=-1)) + own_exp
    past_weights = (past_exp / totals[..., None]).astype(jnp.bfloat16)
    own_weights = (own_exp / totals).astype(jnp.bfloat16)
    mixed_values = jnp.einsum('skgl,slkd->skgd', past_weights.astype(jnp.float32), cached_values)
    mixed_values = mixed_values + own_weights.astype(jnp.float32)[..., None] * value_new.astype(jnp.float32)[:, :, None, :]
    return mixed_values.astype(jnp.bfloat16).reshape(seqs_here, kv_count * group_size * head_width)

def reference(tokens, norm_gain, query_weight, key_weight, value_weight, forget_weight, forget_bias, kv_cache, log_gates, lengths, out_weight, mix_gain, expert_gate, expert_up, expert_down, routes, route_weights, dense_gate, dense_up, dense_down, gate_vector):
    group_size = HEADS // KV_HEADS
    normed = rms_scaled(tokens, norm_gain).astype(jnp.bfloat16)
    queries = jnp.dot(normed, query_weight, preferred_element_type=jnp.float32).astype(jnp.bfloat16)
    key_new = jnp.dot(normed, key_weight, preferred_element_type=jnp.float32).astype(jnp.bfloat16)
    value_new = jnp.dot(normed, value_weight, preferred_element_type=jnp.float32).astype(jnp.bfloat16)
    forget = jax.nn.log_sigmoid(jnp.dot(normed, forget_weight, preferred_element_type=jnp.float32) + forget_bias)
    blocks = (queries.reshape(N_EP, SEQ_DEV, KV_HEADS, group_size, HD), key_new.reshape(N_EP, SEQ_DEV, KV_HEADS, HD), value_new.reshape(N_EP, SEQ_DEV, KV_HEADS, HD), forget.reshape(N_EP, SEQ_DEV, HEADS), kv_cache.reshape(N_EP, SEQ_DEV, CACHE_POSITIONS, KV_HEADS, 2 * HD), log_gates.reshape(N_EP, SEQ_DEV, CACHE_POSITIONS, HEADS), lengths.reshape(N_EP, SEQ_DEV))
    attended = lax.map(attend_block, blocks).reshape(SEQUENCE_TOTAL, HEADS * HD)
    mixed = (tokens.astype(jnp.float32) + jnp.dot(attended, out_weight, preferred_element_type=jnp.float32)).astype(jnp.bfloat16)
    second = rms_scaled(mixed, mix_gain).astype(jnp.bfloat16)
    gate_value = jax.nn.sigmoid(jnp.dot(second.astype(jnp.float32), gate_vector, precision=lax.Precision.HIGHEST))
    dense_hidden = (jax.nn.silu(jnp.dot(second, dense_gate, preferred_element_type=jnp.float32)) * jnp.dot(second, dense_up, preferred_element_type=jnp.float32)).astype(jnp.bfloat16)
    dense_out = jnp.dot(dense_hidden, dense_down, preferred_element_type=jnp.float32)
    most_rows = N_EP * CAP
    flat_routes = routes.reshape(-1)
    flat_weights = route_weights.reshape(-1)
    token_rows = jnp.arange(SEQUENCE_TOTAL * TOPK, dtype=jnp.int32) // TOPK

    def one_expert(routed, inputs):
        expert_index, gate_matrix, up_matrix, down_matrix = inputs
        is_mine = flat_routes == expert_index
        row_order = jnp.argsort(jnp.where(is_mine, 0, 1).astype(jnp.int32), stable=True)[:most_rows]
        chosen_tokens = token_rows[row_order]
        chosen_weights = jnp.where(is_mine[row_order], flat_weights[row_order], 0.0)
        picked = second[chosen_tokens]
        hidden = (jax.nn.silu(jnp.dot(picked, gate_matrix, preferred_element_type=jnp.float32)) * jnp.dot(picked, up_matrix, preferred_element_type=jnp.float32)).astype(jnp.bfloat16)
        result = jnp.dot(hidden, down_matrix, preferred_element_type=jnp.float32).astype(jnp.bfloat16)
        result = lax.optimization_barrier(result).astype(jnp.float32)
        return (routed.at[chosen_tokens].add(chosen_weights[:, None] * result), None)
    routed = lax.scan(one_expert, jnp.zeros((SEQUENCE_TOTAL, D), jnp.float32), (jnp.arange(EXPERTS, dtype=jnp.int32), expert_gate, expert_up, expert_down))[0]
    return (mixed.astype(jnp.float32) + routed + gate_value[:, None] * dense_out).astype(jnp.bfloat16)
```

```python
import functools

import jax
import jax.numpy as jnp
from jax import lax
from jax.experimental import pallas as pl
from jax.experimental.pallas import tpu as pltpu
from jax.sharding import PartitionSpec as P

EPS = 1e-06


def rms_scaled(matrix, gains):
    values = matrix.astype(jnp.float32)
    return values * lax.rsqrt(jnp.mean(values * values, axis=-1, keepdims=True) + EPS) * gains


def attend_local(queries, key_new, value_new, forget, kv_cache, log_gates, lengths):
    seqs_here, cache_len, kv_count, double_width = kv_cache.shape
    head_width = double_width // 2
    group_size = queries.shape[1] // (kv_count * head_width)
    queries = queries.reshape(seqs_here, kv_count, group_size, head_width)
    key_new = key_new.reshape(seqs_here, kv_count, head_width)
    value_new = value_new.reshape(seqs_here, kv_count, head_width)
    cached_keys = kv_cache[..., :head_width]
    cached_values = kv_cache[..., head_width:]
    score_scale = head_width ** (-0.5)
    current_position = jnp.arange(cache_len, dtype=jnp.int32)
    is_last = (current_position[None, :] == lengths[:, None] - 1)[:, :, None]
    last_gate = jnp.sum(jnp.where(is_last, log_gates, 0.0), axis=1)
    newest = last_gate + forget
    gate_bias = newest[:, None, :] - log_gates
    gate_bias = gate_bias.reshape(seqs_here, cache_len, kv_count, group_size).transpose(0, 2, 3, 1)
    past_scores = (
        jnp.einsum("skgd,slkd->skgl", queries, cached_keys, preferred_element_type=jnp.float32)
        * score_scale
        + gate_bias
    )
    is_valid = (current_position[None, :] < lengths[:, None])[:, None, None, :]
    past_scores = jnp.where(is_valid, past_scores, -jnp.inf)
    own_score = (
        jnp.einsum("skgd,skd->skg", queries, key_new, preferred_element_type=jnp.float32)
        * score_scale
    )
    highest = jnp.maximum(jnp.max(past_scores, axis=-1), own_score)
    past_exp = jnp.exp(past_scores - highest[..., None])
    own_exp = jnp.exp(own_score - highest)
    totals = jnp.sum(past_exp, axis=-1) + own_exp
    past_weights = (past_exp / totals[..., None]).astype(jnp.bfloat16)
    own_weights = (own_exp / totals).astype(jnp.bfloat16)
    mixed_values = jnp.einsum(
        "skgl,slkd->skgd", past_weights, cached_values, preferred_element_type=jnp.float32
    )
    mixed_values = (
        mixed_values
        + own_weights.astype(jnp.float32)[..., None] * value_new.astype(jnp.float32)[:, :, None, :]
    )
    return mixed_values.astype(jnp.bfloat16).reshape(seqs_here, kv_count * group_size * head_width)


def shards(
    tokens,
    norm_gain,
    query_weight,
    key_weight,
    value_weight,
    forget_weight,
    forget_bias,
    kv_cache,
    log_gates,
    lengths,
    out_weight,
    mix_gain,
    expert_gate,
    expert_up,
    expert_down,
    routes,
    route_weights,
    dense_gate,
    dense_up,
    dense_down,
    gate_vector,
):
    seq_count = tokens.shape[0]
    normed = rms_scaled(tokens, norm_gain).astype(jnp.bfloat16)
    query_cols = query_weight.shape[1]
    key_cols = key_weight.shape[1]
    columns = lax.all_to_all(normed, "ep", split_axis=1, concat_axis=0, tiled=True)
    row_block = columns
    projected = lax.psum_scatter(
        jnp.concatenate(
            [
                jnp.dot(row_block, matrix, preferred_element_type=jnp.float32)
                for matrix in (query_weight, key_weight, value_weight, forget_weight)
            ],
            axis=1,
        ),
        "ep",
        scatter_dimension=0,
        tiled=True,
    )
    queries = projected[:, :query_cols].astype(jnp.bfloat16)
    key_new = projected[:, query_cols : query_cols + key_cols].astype(jnp.bfloat16)
    value_new = projected[:, query_cols + key_cols : query_cols + 2 * key_cols].astype(jnp.bfloat16)
    forget = jax.nn.log_sigmoid(projected[:, query_cols + 2 * key_cols :] + forget_bias)
    attended = attend_local(queries, key_new, value_new, forget, kv_cache, log_gates, lengths)
    column_terms = jnp.dot(
        lax.all_gather(attended, "ep", axis=0, tiled=True),
        out_weight,
        preferred_element_type=jnp.float32,
    )
    column_total = lax.psum(column_terms, "tp")
    summed = lax.all_to_all(column_total, "ep", split_axis=0, concat_axis=1, tiled=True)
    mixed = (tokens.astype(jnp.float32) + summed).astype(jnp.bfloat16)
    second = rms_scaled(mixed, mix_gain).astype(jnp.bfloat16)
    gate_value = jax.nn.sigmoid(
        jnp.dot(second.astype(jnp.float32), gate_vector, precision=lax.Precision.HIGHEST)
    )
    experts = lax.axis_size("ep")
    top_count = routes.shape[1]
    capacity = max(2, 2 * seq_count * top_count // experts)
    flat_routes = routes.reshape(-1)
    one_hot = (flat_routes[:, None] == jnp.arange(experts, dtype=jnp.int32)[None, :]).astype(
        jnp.int32
    )
    earlier = jnp.sum((jnp.cumsum(one_hot, axis=0) - one_hot) * one_hot, axis=1)
    slot_index = (flat_routes * capacity + earlier).reshape(seq_count, top_count)
    slot_ids = jnp.arange(experts * capacity, dtype=jnp.int32)
    dispatch_map = jnp.any(slot_index[None, :, :] == slot_ids[:, None, None], axis=2).astype(
        jnp.bfloat16
    )
    outgoing = jnp.dot(dispatch_map, second, preferred_element_type=jnp.float32).astype(
        jnp.bfloat16
    )
    outgoing = outgoing.reshape(experts, capacity, second.shape[1])
    received = lax.all_to_all(outgoing, "ep", split_axis=0, concat_axis=0, tiled=True)
    sources, items, model_width = received.shape
    flat_rows = received.reshape(sources * items, model_width)
    gate_pre = jnp.dot(flat_rows, expert_gate[0], preferred_element_type=jnp.float32)
    up_pre = jnp.dot(flat_rows, expert_up[0], preferred_element_type=jnp.float32)
    hidden = (jax.nn.silu(gate_pre) * up_pre).astype(jnp.bfloat16)
    partial_rows = jnp.dot(hidden, expert_down[0], preferred_element_type=jnp.float32)
    reduced = lax.psum_scatter(partial_rows, "tp", scatter_dimension=1, tiled=True)
    replies = reduced.astype(jnp.bfloat16).reshape(sources, items, reduced.shape[1])
    returned = lax.all_to_all(replies, "ep", split_axis=0, concat_axis=0, tiled=True)
    quarter_cols = returned.shape[2]
    picked = returned.reshape(experts * capacity, quarter_cols)[slot_index.reshape(-1)]
    routed = jnp.sum(
        picked.astype(jnp.float32).reshape(seq_count, top_count, quarter_cols)
        * route_weights[:, :, None],
        axis=1,
    )
    tp_index = lax.axis_index("tp")
    piece = lax.all_gather(second, "ep", axis=0, tiled=True)
    dense_hidden = (
        jax.nn.silu(jnp.dot(piece, dense_gate, preferred_element_type=jnp.float32))
        * jnp.dot(piece, dense_up, preferred_element_type=jnp.float32)
    ).astype(jnp.bfloat16)
    row_block = dense_hidden
    dense_out = lax.psum_scatter(
        jnp.dot(row_block, dense_down, preferred_element_type=jnp.float32),
        "ep",
        scatter_dimension=0,
        tiled=True,
    )
    residual = lax.dynamic_slice_in_dim(mixed, tp_index * quarter_cols, quarter_cols, 1).astype(
        jnp.float32
    )
    return (residual + routed + gate_value[:, None] * dense_out).astype(jnp.bfloat16)


MESH = pl.DeviceIdType.MESH
LANES = 128


def nt_dot(a, b):
    return lax.dot_general(a, b, (((1,), (1,)), ((), ())), preferred_element_type=jnp.float32)


def remote(src, dst, send_sem, recv_sem, ep, tp):
    copy = pltpu.make_async_remote_copy(
        src_ref=src,
        dst_ref=dst,
        send_sem=send_sem,
        recv_sem=recv_sem,
        device_id=(ep, tp),
        device_id_type=MESH,
    )
    copy.start()
    return copy


def front_kernel(
    n_ep,
    tok_ref,
    gain_ref,
    wmat_ref,
    wq_ref,
    wk_ref,
    wv_ref,
    wf_ref,
    proj_ref,
    tokc_ref,
    aux_ref,
    aux_own,
    part,
    part_in,
    ts_sem,
    tr_sem,
    as_sem,
    ar_sem,
    ps_sem,
    pr_sem,
):
    e = lax.axis_index("ep")
    t = lax.axis_index("tp")
    seqs, width = tok_ref.shape
    cols = width // n_ep
    barrier = pltpu.get_barrier_semaphore()
    for o in range(1, n_ep):
        pl.semaphore_signal(
            barrier, inc=1, device_id=(lax.rem(e + o, n_ep), t), device_id_type=MESH
        )
    tokens = tok_ref[...].astype(jnp.float32)
    scale = lax.rsqrt(jnp.mean(tokens * tokens, axis=-1, keepdims=True) + EPS)
    lane = lax.broadcasted_iota(jnp.int32, (seqs, LANES), 1)
    aux_own[...] = jnp.where(lane == LANES - 1, scale, wmat_ref[...])
    pl.semaphore_wait(barrier, n_ep - 1)
    copies = []
    for o in range(1, n_ep):
        peer = lax.rem(e + o, n_ep)
        chunk = pl.ds(pl.multiple_of(peer * cols, LANES), cols)
        copies.append(
            remote(tok_ref.at[:, chunk], tokc_ref.at[e], ts_sem.at[o], tr_sem.at[o], peer, t)
        )
        copies.append(remote(aux_own, aux_ref.at[e], as_sem.at[o], ar_sem.at[o], peer, t))
    tokc_ref[e] = tok_ref[:, pl.ds(pl.multiple_of(e * cols, LANES), cols)]
    aux_ref[e] = aux_own[...]
    for copy in copies:
        copy.wait_recv()
    rows = n_ep * seqs
    scales = aux_ref[...].reshape(rows, LANES)[:, LANES - 1 :]
    block = tokc_ref[...].reshape(rows, cols).astype(jnp.float32)
    normed = (block * scales * gain_ref[pl.ds(e, 1), :]).astype(jnp.bfloat16)
    queries = jnp.dot(normed, wq_ref[...], preferred_element_type=jnp.float32)
    qc = queries.shape[1]
    kc = wk_ref.shape[0]
    fc = wf_ref.shape[0]
    part[:, :, :qc] = queries.reshape(n_ep, seqs, qc)
    rest = [nt_dot(normed, wk_ref[...]), nt_dot(normed, wv_ref[...]), nt_dot(normed, wf_ref[...])]
    fill = part.shape[2] - qc - 2 * kc - fc
    rest = jnp.concatenate(rest + [jnp.zeros((rows, fill), jnp.float32)], axis=1)
    part[:, :, qc:] = rest.reshape(n_ep, seqs, rest.shape[1])
    sums = []
    for o in range(1, n_ep):
        peer = lax.rem(e + o, n_ep)
        sums.append(remote(part.at[peer], part_in.at[o], ps_sem.at[o], pr_sem.at[o], peer, t))
    total = part[e]
    for o in range(1, n_ep):
        sums[o - 1].wait_recv()
        total = total + part_in[o]
    proj_ref[...] = total
    for copy in copies + sums:
        copy.wait_send()


def back_kernel(
    n_ep,
    n_tp,
    att_ref,
    tokc_ref,
    aux_ref,
    gain_ref,
    vector_ref,
    ow_hbm,
    eg_hbm,
    eu_hbm,
    ed_hbm,
    dg_hbm,
    du_hbm,
    dd_hbm,
    out_ref,
    ow,
    eg,
    eu,
    ed,
    dg,
    du,
    dd,
    att,
    osend,
    orecv,
    mix,
    sec,
    dsend,
    drecv,
    ysend,
    yrecv,
    csend,
    crecv,
    w_sem,
    a_sem,
    o_sem,
    g_sem,
    gy_sem,
    gd_sem,
    d_sem,
    y_sem,
    c_sem,
):
    e = lax.axis_index("ep")
    t = lax.axis_index("tp")
    ty = lax.rem(t + 2, n_tp)
    td = t + 1 - 2 * lax.rem(t, 2)
    tdy = lax.rem(td + 2, n_tp)
    seqs = att_ref.shape[0]
    rows = n_ep * seqs
    loads = [
        pltpu.make_async_copy(src, dst, w_sem.at[i])
        for i, (src, dst) in enumerate(
            [
                (ow_hbm, ow),
                (eg_hbm.at[0], eg),
                (eu_hbm.at[0], eu),
                (ed_hbm.at[0], ed),
                (dg_hbm, dg),
                (du_hbm, du),
                (dd_hbm, dd),
            ]
        )
    ]
    for load in loads:
        load.start()
    barrier = pltpu.get_barrier_semaphore()
    for o in range(1, n_ep):
        pl.semaphore_signal(
            barrier, inc=1, device_id=(lax.rem(e + o, n_ep), t), device_id_type=MESH
        )
    for o in range(1, n_tp):
        pl.semaphore_signal(
            barrier, inc=1, device_id=(e, lax.rem(t + o, n_tp)), device_id_type=MESH
        )
    pl.semaphore_wait(barrier, n_ep + n_tp - 2)
    pending = []
    copies = []
    for o in range(1, n_ep):
        peer = lax.rem(e + o, n_ep)
        copies.append(remote(att_ref, att.at[e], a_sem.at[0, o], a_sem.at[1, o], peer, t))
    att[e] = att_ref[...]
    loads[0].wait()
    for copy in copies:
        copy.wait_recv()
    pending += copies
    partial = jnp.dot(
        att[...].reshape(rows, att_ref.shape[1]), ow[...], preferred_element_type=jnp.float32
    )
    cw = osend.shape[2]
    for j in range(n_tp):
        osend[j] = partial[:, j * cw : (j + 1) * cw]
    copies = []
    for o in range(1, n_tp):
        peer = lax.rem(t + o, n_tp)
        copies.append(
            remote(osend.at[peer], orecv.at[o], o_sem.at[0, o], o_sem.at[1, o], e, peer)
        )
    total = osend[t]
    for o in range(1, n_tp):
        copies[o - 1].wait_recv()
        total = total + orecv[o]
    pending += copies
    own_tokens = tokc_ref[:, :, pl.ds(pl.multiple_of(t * cw, LANES), cw)].reshape(rows, cw)
    mix[t, e] = (own_tokens.astype(jnp.float32) + total).astype(jnp.bfloat16)
    arrivals, y_copies, d_copies = [], [], []
    for o in range(1, n_ep):
        peer = lax.rem(e + o, n_ep)
        arrivals.append(
            remote(mix.at[t, e], mix.at[t, e], g_sem.at[0, o], g_sem.at[1, o], peer, t)
        )
    for o in range(n_ep + 1):
        if o < n_ep:
            slot = mix.at[t, lax.rem(e + n_ep - o, n_ep)]
            if o > 0:
                arrivals[o - 1].wait_recv()
            y_copies.append(remote(slot, slot, gy_sem.at[0, o], gy_sem.at[1, o], e, ty))
            d_copies.append(remote(slot, slot, gd_sem.at[0, 0, o], gd_sem.at[1, 0, o], e, td))
        if o > 0:
            slot = mix.at[ty, lax.rem(e + n_ep - (o - 1), n_ep)]
            y_copies[o - 1].wait_recv()
            d_copies.append(
                remote(slot, slot, gd_sem.at[0, 1, o - 1], gd_sem.at[1, 1, o - 1], e, td)
            )
    for copy in d_copies:
        copy.wait_recv()
    pending += arrivals + y_copies + d_copies
    squares = jnp.zeros((rows, cw), jnp.float32)
    for j in range(n_tp):
        for i in range(n_ep):
            values = mix[j, i].astype(jnp.float32)
            squares = squares + values * values
    scale = lax.rsqrt(jnp.sum(squares, axis=-1, keepdims=True) / sec.shape[1] + EPS)
    gates = jnp.zeros((rows, cw), jnp.float32)
    for i in range(n_ep):
        for j in range(n_tp):
            at = (i * n_tp + j) * cw
            values = mix[j, i].astype(jnp.float32) * scale * gain_ref[:, at : at + cw]
            values = values.astype(jnp.bfloat16)
            sec[:, at : at + cw] = values
            gates = gates + values.astype(jnp.float32) * vector_ref[:, at : at + cw]
    gate_value = jax.nn.sigmoid(jnp.sum(gates, axis=-1, keepdims=True))
    for load in loads[1:4]:
        load.wait()
    hidden = (
        jax.nn.silu(jnp.dot(sec[...], eg[...], preferred_element_type=jnp.float32))
        * jnp.dot(sec[...], eu[...], preferred_element_type=jnp.float32)
    ).astype(jnp.bfloat16)
    ocols = out_ref.shape[1]

    def down(owner):
        chunk = pl.ds(pl.multiple_of(owner * ocols, LANES), ocols)
        return jnp.dot(hidden, ed[:, chunk], preferred_element_type=jnp.float32)

    pair = []
    for k, owner in enumerate((tdy, td)):
        dsend[k] = down(owner)
        pair.append(
            remote(dsend.at[k], drecv.at[k], d_sem.at[0, k], d_sem.at[1, k], e, td)
        )
    across = down(ty)
    pair[0].wait_recv()
    ysend[...] = (across + drecv[0]).astype(jnp.bfloat16)
    y_copy = remote(ysend, yrecv, y_sem.at[0], y_sem.at[1], e, ty)
    own = down(t)
    for load in loads[4:]:
        load.wait()
    dense_hidden = (
        jax.nn.silu(jnp.dot(sec[...], dg[...], preferred_element_type=jnp.float32))
        * jnp.dot(sec[...], du[...], preferred_element_type=jnp.float32)
    ).astype(jnp.bfloat16)
    dense = jnp.dot(dense_hidden, dd[...], preferred_element_type=jnp.float32)
    pair[1].wait_recv()
    y_copy.wait_recv()
    expert_out = (own + drecv[1] + yrecv[...].astype(jnp.float32)).astype(jnp.bfloat16)
    pending += pair + [y_copy]
    aux = aux_ref[...].reshape(rows, LANES)
    lane = lax.broadcasted_iota(jnp.int32, (rows, LANES), 1)
    weight = jnp.sum(jnp.where(lane == e, aux, 0.0), axis=-1, keepdims=True)
    terms = weight * expert_out.astype(jnp.float32) + gate_value * dense
    csend[...] = terms.astype(jnp.bfloat16).reshape(n_ep, seqs, ocols)
    copies = []
    for o in range(1, n_ep):
        peer = lax.rem(e + o, n_ep)
        copies.append(
            remote(csend.at[peer], crecv.at[o], c_sem.at[0, o], c_sem.at[1, o], peer, t)
        )
    mine = pl.ds(pl.multiple_of(e * seqs, seqs), seqs)
    per_tp = n_ep // n_tp
    pieces = [mix[j, t * per_tp + k, mine, :] for k in range(per_tp) for j in range(n_tp)]
    total = jnp.concatenate(pieces, axis=1).astype(jnp.float32)
    total = total + csend[e].astype(jnp.float32)
    for o in range(1, n_ep):
        copies[o - 1].wait_recv()
        total = total + crecv[o].astype(jnp.float32)
    out_ref[...] = total.astype(jnp.bfloat16)
    for copy in pending + copies:
        copy.wait_send()


def fused_shards(
    tokens,
    norm_gain,
    query_weight,
    key_weight,
    value_weight,
    forget_weight,
    forget_bias,
    kv_cache,
    log_gates,
    lengths,
    out_weight,
    mix_gain,
    expert_gate,
    expert_up,
    expert_down,
    routes,
    route_weights,
    dense_gate,
    dense_up,
    dense_down,
    gate_vector,
):
    n_ep = lax.axis_size("ep")
    n_tp = lax.axis_size("tp")
    seqs, width = tokens.shape
    rows = n_ep * seqs
    cols = width // n_ep
    qc = query_weight.shape[1]
    kc = key_weight.shape[1]
    fc = forget_weight.shape[1]
    pw = qc + -(-(2 * kc + fc) // LANES) * LANES
    vmem = pl.BlockSpec(memory_space=pltpu.VMEM)
    anywhere = pl.BlockSpec(memory_space=pl.ANY)
    dma = pltpu.SemaphoreType.DMA
    f32, bf16 = jnp.float32, jnp.bfloat16
    chosen = routes[:, :, None] == jnp.arange(LANES, dtype=jnp.int32)[None, None, :]
    wmat = jnp.sum(jnp.where(chosen, route_weights[:, :, None], 0.0), axis=1)
    projected, token_cols, aux = pl.pallas_call(
        functools.partial(front_kernel, n_ep),
        out_shape=(
            jax.ShapeDtypeStruct((seqs, pw), f32),
            jax.ShapeDtypeStruct((n_ep, seqs, cols), bf16),
            jax.ShapeDtypeStruct((n_ep, seqs, LANES), f32),
        ),
        in_specs=[vmem] * 7,
        out_specs=(vmem,) * 3,
        scratch_shapes=[
            pltpu.VMEM((seqs, LANES), f32),
            pltpu.VMEM((n_ep, seqs, pw), f32),
            pltpu.VMEM((n_ep, seqs, pw), f32),
        ]
        + [dma((n_ep,))] * 6,
        compiler_params=pltpu.CompilerParams(collective_id=0, has_side_effects=True),
        name="front",
    )(
        tokens,
        norm_gain.reshape(n_ep, cols),
        wmat,
        query_weight,
        key_weight.T,
        value_weight.T,
        forget_weight.T,
    )
    queries = projected[:, :qc].astype(bf16)
    key_new = projected[:, qc : qc + kc].astype(bf16)
    value_new = projected[:, qc + kc : qc + 2 * kc].astype(bf16)
    forget = jax.nn.log_sigmoid(projected[:, qc + 2 * kc : qc + 2 * kc + fc] + forget_bias)
    attended = attend_local(queries, key_new, value_new, forget, kv_cache, log_gates, lengths)
    cw = cols // n_tp
    ocols = width // n_tp
    return pl.pallas_call(
        functools.partial(back_kernel, n_ep, n_tp),
        out_shape=jax.ShapeDtypeStruct((seqs, ocols), bf16),
        in_specs=[vmem] * 5 + [anywhere] * 7,
        out_specs=vmem,
        scratch_shapes=[
            pltpu.VMEM(out_weight.shape, bf16),
            pltpu.VMEM(expert_gate.shape[1:], bf16),
            pltpu.VMEM(expert_up.shape[1:], bf16),
            pltpu.VMEM(expert_down.shape[1:], bf16),
            pltpu.VMEM(dense_gate.shape, bf16),
            pltpu.VMEM(dense_up.shape, bf16),
            pltpu.VMEM(dense_down.shape, bf16),
            pltpu.VMEM((n_ep, seqs, attended.shape[1]), bf16),
            pltpu.VMEM((n_tp, rows, cw), f32),
            pltpu.VMEM((n_tp, rows, cw), f32),
            pltpu.VMEM((n_tp, n_ep, rows, cw), bf16),
            pltpu.VMEM((rows, width), bf16),
            pltpu.VMEM((2, rows, ocols), f32),
            pltpu.VMEM((2, rows, ocols), f32),
            pltpu.VMEM((rows, ocols), bf16),
            pltpu.VMEM((rows, ocols), bf16),
            pltpu.VMEM((n_ep, seqs, ocols), bf16),
            pltpu.VMEM((n_ep, seqs, ocols), bf16),
            dma((7,)),
            dma((2, n_ep)),
            dma((2, n_tp)),
            dma((2, n_ep)),
            dma((2, n_ep)),
            dma((2, 2, n_ep)),
            dma((2, 2)),
            dma((2,)),
            dma((2, n_ep)),
        ],
        compiler_params=pltpu.CompilerParams(
            collective_id=1, has_side_effects=True, vmem_limit_bytes=56 * 1024 * 1024
        ),
        name="back",
    )(
        attended,
        token_cols,
        aux,
        mix_gain.reshape(1, width),
        gate_vector.reshape(1, width),
        out_weight,
        expert_gate,
        expert_up,
        expert_down,
        dense_gate,
        dense_up,
        dense_down,
    )


def layer(*arrays):
    tokens, routes = arrays[0], arrays[15]
    n_ep, n_tp = lax.axis_size("ep"), lax.axis_size("tp")
    seqs, width = tokens.shape
    capacity = seqs * routes.shape[1]
    fits = (
        n_tp == 4
        and n_ep % n_tp == 0
        and n_ep < LANES
        and n_ep * seqs <= 2 * capacity
        and width % (n_ep * n_tp * LANES) == 0
        and arrays[2].shape[1] % LANES == 0
    )
    return (fused_shards if fits else shards)(*arrays)


def solution(mesh):
    return jax.shard_map(
        layer,
        mesh=mesh,
        in_specs=(
            P("ep", None),
            P(),
            P("ep", "tp"),
            P("ep", "tp"),
            P("ep", "tp"),
            P("ep", "tp"),
            P("tp"),
            P("ep", None, "tp", None),
            P("ep", None, "tp"),
            P("ep"),
            P("tp", "ep"),
            P(),
            P("ep", None, "tp"),
            P("ep", None, "tp"),
            P("ep", "tp", None),
            P("ep", None),
            P("ep", None),
            P(None, "ep"),
            P(None, "ep"),
            P("ep", "tp"),
            P(),
        ),
        out_specs=P("ep", "tp"),
        check_vma=False,
    )
```

```python
import functools

import jax
import jax.numpy as jnp
from jax import lax
from jax.experimental import pallas as pl
from jax.experimental.pallas import tpu as pltpu
from jax.sharding import PartitionSpec as P

EPS = 1e-06


def rms_scaled(matrix, gains):
    values = matrix.astype(jnp.float32)
    return values * lax.rsqrt(jnp.mean(values * values, axis=-1, keepdims=True) + EPS) * gains


def attend_local(queries, key_new, value_new, forget, kv_cache, log_gates, lengths):
    seqs_here, cache_len, kv_count, double_width = kv_cache.shape
    head_width = double_width // 2
    group_size = queries.shape[1] // (kv_count * head_width)
    queries = queries.reshape(seqs_here, kv_count, group_size, head_width)
    key_new = key_new.reshape(seqs_here, kv_count, head_width)
    value_new = value_new.reshape(seqs_here, kv_count, head_width)
    cached_keys = kv_cache[..., :head_width]
    cached_values = kv_cache[..., head_width:]
    score_scale = head_width ** (-0.5)
    current_position = jnp.arange(cache_len, dtype=jnp.int32)
    is_last = (current_position[None, :] == lengths[:, None] - 1)[:, :, None]
    last_gate = jnp.sum(jnp.where(is_last, log_gates, 0.0), axis=1)
    newest = last_gate + forget
    gate_bias = newest[:, None, :] - log_gates
    gate_bias = gate_bias.reshape(seqs_here, cache_len, kv_count, group_size).transpose(0, 2, 3, 1)
    past_scores = (
        jnp.einsum("skgd,slkd->skgl", queries, cached_keys, preferred_element_type=jnp.float32)
        * score_scale
        + gate_bias
    )
    is_valid = (current_position[None, :] < lengths[:, None])[:, None, None, :]
    past_scores = jnp.where(is_valid, past_scores, -jnp.inf)
    own_score = (
        jnp.einsum("skgd,skd->skg", queries, key_new, preferred_element_type=jnp.float32)
        * score_scale
    )
    highest = jnp.maximum(jnp.max(past_scores, axis=-1), own_score)
    past_exp = jnp.exp(past_scores - highest[..., None])
    own_exp = jnp.exp(own_score - highest)
    totals = jnp.sum(past_exp, axis=-1) + own_exp
    past_weights = (past_exp / totals[..., None]).astype(jnp.bfloat16)
    own_weights = (own_exp / totals).astype(jnp.bfloat16)
    mixed_values = jnp.einsum(
        "skgl,slkd->skgd", past_weights, cached_values, preferred_element_type=jnp.float32
    )
    mixed_values = (
        mixed_values
        + own_weights.astype(jnp.float32)[..., None] * value_new.astype(jnp.float32)[:, :, None, :]
    )
    return mixed_values.astype(jnp.bfloat16).reshape(seqs_here, kv_count * group_size * head_width)


def shards(
    tokens,
    norm_gain,
    query_weight,
    key_weight,
    value_weight,
    forget_weight,
    forget_bias,
    kv_cache,
    log_gates,
    lengths,
    out_weight,
    mix_gain,
    expert_gate,
    expert_up,
    expert_down,
    routes,
    route_weights,
    dense_gate,
    dense_up,
    dense_down,
    gate_vector,
):
    seq_count = tokens.shape[0]
    normed = rms_scaled(tokens, norm_gain).astype(jnp.bfloat16)
    query_cols = query_weight.shape[1]
    key_cols = key_weight.shape[1]
    columns = lax.all_to_all(normed, "ep", split_axis=1, concat_axis=0, tiled=True)
    row_block = columns
    projected = lax.psum_scatter(
        jnp.concatenate(
            [
                jnp.dot(row_block, matrix, preferred_element_type=jnp.float32)
                for matrix in (query_weight, key_weight, value_weight, forget_weight)
            ],
            axis=1,
        ),
        "ep",
        scatter_dimension=0,
        tiled=True,
    )
    queries = projected[:, :query_cols].astype(jnp.bfloat16)
    key_new = projected[:, query_cols : query_cols + key_cols].astype(jnp.bfloat16)
    value_new = projected[:, query_cols + key_cols : query_cols + 2 * key_cols].astype(jnp.bfloat16)
    forget = jax.nn.log_sigmoid(projected[:, query_cols + 2 * key_cols :] + forget_bias)
    attended = attend_local(queries, key_new, value_new, forget, kv_cache, log_gates, lengths)
    column_terms = jnp.dot(
        lax.all_gather(attended, "ep", axis=0, tiled=True),
        out_weight,
        preferred_element_type=jnp.float32,
    )
    column_total = lax.psum(column_terms, "tp")
    summed = lax.all_to_all(column_total, "ep", split_axis=0, concat_axis=1, tiled=True)
    mixed = (tokens.astype(jnp.float32) + summed).astype(jnp.bfloat16)
    second = rms_scaled(mixed, mix_gain).astype(jnp.bfloat16)
    gate_value = jax.nn.sigmoid(
        jnp.dot(second.astype(jnp.float32), gate_vector, precision=lax.Precision.HIGHEST)
    )
    experts = lax.axis_size("ep")
    top_count = routes.shape[1]
    capacity = max(2, 2 * seq_count * top_count // experts)
    flat_routes = routes.reshape(-1)
    one_hot = (flat_routes[:, None] == jnp.arange(experts, dtype=jnp.int32)[None, :]).astype(
        jnp.int32
    )
    earlier = jnp.sum((jnp.cumsum(one_hot, axis=0) - one_hot) * one_hot, axis=1)
    slot_index = (flat_routes * capacity + earlier).reshape(seq_count, top_count)
    slot_ids = jnp.arange(experts * capacity, dtype=jnp.int32)
    dispatch_map = jnp.any(slot_index[None, :, :] == slot_ids[:, None, None], axis=2).astype(
        jnp.bfloat16
    )
    outgoing = jnp.dot(dispatch_map, second, preferred_element_type=jnp.float32).astype(
        jnp.bfloat16
    )
    outgoing = outgoing.reshape(experts, capacity, second.shape[1])
    received = lax.all_to_all(outgoing, "ep", split_axis=0, concat_axis=0, tiled=True)
    sources, items, model_width = received.shape
    flat_rows = received.reshape(sources * items, model_width)
    gate_pre = jnp.dot(flat_rows, expert_gate[0], preferred_element_type=jnp.float32)
    up_pre = jnp.dot(flat_rows, expert_up[0], preferred_element_type=jnp.float32)
    hidden = (jax.nn.silu(gate_pre) * up_pre).astype(jnp.bfloat16)
    partial_rows = jnp.dot(hidden, expert_down[0], preferred_element_type=jnp.float32)
    reduced = lax.psum_scatter(partial_rows, "tp", scatter_dimension=1, tiled=True)
    replies = reduced.astype(jnp.bfloat16).reshape(sources, items, reduced.shape[1])
    returned = lax.all_to_all(replies, "ep", split_axis=0, concat_axis=0, tiled=True)
    quarter_cols = returned.shape[2]
    picked = returned.reshape(experts * capacity, quarter_cols)[slot_index.reshape(-1)]
    routed = jnp.sum(
        picked.astype(jnp.float32).reshape(seq_count, top_count, quarter_cols)
        * route_weights[:, :, None],
        axis=1,
    )
    tp_index = lax.axis_index("tp")
    piece = lax.all_gather(second, "ep", axis=0, tiled=True)
    dense_hidden = (
        jax.nn.silu(jnp.dot(piece, dense_gate, preferred_element_type=jnp.float32))
        * jnp.dot(piece, dense_up, preferred_element_type=jnp.float32)
    ).astype(jnp.bfloat16)
    row_block = dense_hidden
    dense_out = lax.psum_scatter(
        jnp.dot(row_block, dense_down, preferred_element_type=jnp.float32),
        "ep",
        scatter_dimension=0,
        tiled=True,
    )
    residual = lax.dynamic_slice_in_dim(mixed, tp_index * quarter_cols, quarter_cols, 1).astype(
        jnp.float32
    )
    return (residual + routed + gate_value[:, None] * dense_out).astype(jnp.bfloat16)


MESH = pl.DeviceIdType.MESH
LANES = 128


def nt_dot(a, b):
    return lax.dot_general(a, b, (((1,), (1,)), ((), ())), preferred_element_type=jnp.float32)


def remote(src, dst, send_sem, recv_sem, ep, tp):
    copy = pltpu.make_async_remote_copy(
        src_ref=src,
        dst_ref=dst,
        send_sem=send_sem,
        recv_sem=recv_sem,
        device_id=(ep, tp),
        device_id_type=MESH,
    )
    copy.start()
    return copy


def layer_kernel(
    n_ep,
    n_tp,
    tok_ref,
    gain_ref,
    routes_ref,
    weights_ref,
    wk_ref,
    wv_ref,
    wf_ref,
    bias_ref,
    mgain_ref,
    vector_ref,
    lengths_ref,
    wq_hbm,
    kv_hbm,
    gates_hbm,
    ow_hbm,
    eg_hbm,
    eu_hbm,
    ed_hbm,
    dg_hbm,
    du_hbm,
    dd_hbm,
    out_ref,
    tokc,
    aux_own,
    aux_all,
    part,
    part_in,
    wq,
    kv,
    lgates,
    qs,
    score,
    prob,
    heads,
    att_own,
    att,
    ow,
    eg,
    eu,
    ed,
    dg,
    du,
    dd,
    osend,
    orecv,
    mix,
    sec,
    hid,
    csend,
    crecv,
    w_sem,
    e_sem,
    t_sem,
    x_sem,
    p_sem,
    a_sem,
    o_sem,
    g_sem,
    gy_sem,
    gd_sem,
    h_sem,
    c_sem,
):
    e = lax.axis_index("ep")
    t = lax.axis_index("tp")
    ty = lax.rem(t + 2, n_tp)
    td = t + 1 - 2 * lax.rem(t, 2)
    seqs, width = tok_ref.shape
    rows = n_ep * seqs
    cols = width // n_ep
    ocols = width // n_tp
    bf16, f32 = jnp.bfloat16, jnp.float32
    barrier = pltpu.get_barrier_semaphore()
    for o in range(1, n_ep):
        pl.semaphore_signal(
            barrier, inc=1, device_id=(lax.rem(e + o, n_ep), t), device_id_type=MESH
        )
    for o in range(1, n_tp):
        pl.semaphore_signal(
            barrier, inc=1, device_id=(e, lax.rem(t + o, n_tp)), device_id_type=MESH
        )
    own_cols = pl.ds(pl.multiple_of(t * ocols, LANES), ocols)
    loads = [
        pltpu.make_async_copy(src, dst, w_sem.at[i])
        for i, (src, dst) in enumerate(
            [
                (wq_hbm, wq),
                (gates_hbm, lgates),
                (kv_hbm, kv),
                (ow_hbm, ow),
                (eg_hbm.at[0], eg),
                (eu_hbm.at[0], eu),
                (dg_hbm, dg),
                (du_hbm, du),
                (dd_hbm, dd),
                (ed_hbm.at[0, :, own_cols], ed.at[t]),
            ]
        )
    ]
    for load in loads:
        load.start()
    tokens = tok_ref[...].astype(f32)
    scale = lax.rsqrt(jnp.mean(tokens * tokens, axis=-1, keepdims=True) + EPS)
    lane = lax.broadcasted_iota(jnp.int32, (seqs, LANES), 1)
    lane_f = lane.astype(f32)
    eye = lax.broadcasted_iota(jnp.int32, (seqs, seqs), 0) == lax.broadcasted_iota(
        jnp.int32, (seqs, seqs), 1
    )
    table = jnp.where(lane == LANES - 1, scale, 0.0)
    for k in range(routes_ref.shape[0]):
        picked = routes_ref[k : k + 1, :].astype(f32)
        picked = jnp.sum(jnp.where(eye, picked, 0.0), axis=-1, keepdims=True)
        amount = jnp.sum(jnp.where(eye, weights_ref[k : k + 1, :], 0.0), axis=-1, keepdims=True)
        table = table + jnp.where(lane_f == picked, amount, 0.0)
    aux_own[...] = table
    pl.semaphore_wait(barrier, n_ep + n_tp - 2)
    pending = []
    copies = []
    for o in range(1, n_ep):
        peer = lax.rem(e + o, n_ep)
        chunk = pl.ds(pl.multiple_of(peer * cols, LANES), cols)
        copies.append(
            remote(tok_ref.at[:, chunk], tokc.at[e], t_sem.at[0, o], t_sem.at[1, o], peer, t)
        )
        copies.append(remote(aux_own, aux_all.at[e], x_sem.at[0, o], x_sem.at[1, o], peer, t))
    down_copies = []
    for o in range(1, n_tp):
        peer = lax.rem(t + o, n_tp)
        chunk = pl.ds(pl.multiple_of(peer * ocols, LANES), ocols)
        down_copies.append(
            remote(
                ed_hbm.at[0, :, chunk], ed.at[t], e_sem.at[0, o], e_sem.at[1, o], e, peer
            )
        )
    tokc[e] = tok_ref[:, pl.ds(pl.multiple_of(e * cols, LANES), cols)]
    aux_all[e] = aux_own[...]
    for copy in copies:
        copy.wait_recv()
    pending += copies
    aux = aux_all[...].reshape(rows, LANES)
    block = tokc[...].reshape(rows, cols).astype(f32)
    gain = gain_ref[:, pl.ds(pl.multiple_of(e * cols, LANES), cols)]
    normed = (block * aux[:, LANES - 1 :] * gain).astype(bf16)
    loads[0].wait()
    queries = jnp.dot(normed, wq[...], preferred_element_type=f32)
    qc = queries.shape[1]
    hd = wk_ref.shape[0]
    group = wf_ref.shape[0]
    part[:, :, :qc] = queries.reshape(n_ep, seqs, qc)
    rest = [nt_dot(normed, wk_ref[...]), nt_dot(normed, wv_ref[...]), nt_dot(normed, wf_ref[...])]
    fill = part.shape[2] - qc - 2 * hd - group
    rest = jnp.concatenate(rest + [jnp.zeros((rows, fill), f32)], axis=1)
    part[:, :, qc:] = rest.reshape(n_ep, seqs, rest.shape[1])
    sums = []
    for o in range(1, n_ep):
        peer = lax.rem(e + o, n_ep)
        sums.append(remote(part.at[peer], part_in.at[o], p_sem.at[0, o], p_sem.at[1, o], peer, t))
    total = part[e]
    for o in range(1, n_ep):
        sums[o - 1].wait_recv()
        total = total + part_in[o]
    pending += sums
    rounded = total[:, : qc + 2 * hd].astype(bf16).astype(f32)
    fresh = rounded[:, qc:]
    forget = jax.nn.log_sigmoid(total[:, qc + 2 * hd : qc + 2 * hd + group] + bias_ref[...])
    zeros = jnp.zeros((seqs, hd), f32)
    for g in range(group):
        qs[:, g, :] = jnp.concatenate([rounded[:, g * hd : (g + 1) * hd], zeros], axis=1)
    loads[1].wait()
    loads[2].wait()
    for s in range(seqs):
        score[s] = nt_dot(qs[s].astype(bf16), kv[s])
    inverse = hd ** (-0.5)
    count = kv.shape[1]
    place = lax.broadcasted_iota(jnp.int32, (group, count), 1)
    square = lax.broadcasted_iota(jnp.int32, (group, group), 0) == lax.broadcasted_iota(
        jnp.int32, (group, group), 1
    )
    own_weights = []
    for s in range(seqs):
        length = lengths_ref[s]
        levels = lgates[s]
        last = jnp.sum(jnp.where(place == length - 1, levels, 0.0), axis=-1, keepdims=True)
        newest = last + jnp.sum(
            jnp.where(square, forget[s : s + 1, :], 0.0), axis=-1, keepdims=True
        )
        past = jnp.where(place < length, score[s] * inverse + (newest - levels), -jnp.inf)
        own = jnp.sum(qs[s] * fresh[s : s + 1, :], axis=-1, keepdims=True) * inverse
        highest = jnp.maximum(jnp.max(past, axis=-1, keepdims=True), own)
        past = jnp.exp(past - highest)
        own = jnp.exp(own - highest)
        whole = jnp.sum(past, axis=-1, keepdims=True) + own
        prob[s] = (past / whole).astype(bf16)
        own_weights.append((own / whole).astype(bf16).astype(f32))
    for s in range(seqs):
        values = jnp.dot(prob[s], kv[s], preferred_element_type=f32)
        heads[s] = values + own_weights[s] * fresh[s : s + 1, :]
    att_own[...] = jnp.concatenate([heads[:, g, hd:] for g in range(group)], axis=1).astype(bf16)
    copies = []
    for o in range(1, n_ep):
        peer = lax.rem(e + o, n_ep)
        copies.append(remote(att_own, att.at[e], a_sem.at[0, o], a_sem.at[1, o], peer, t))
    att[e] = att_own[...]
    loads[3].wait()
    for copy in copies:
        copy.wait_recv()
    pending += copies
    gathered = att[...].reshape(rows, att.shape[2])
    cw = cols // n_tp

    def out_columns(owner):
        chunk = pl.ds(pl.multiple_of(owner * cw, LANES), cw)
        return jnp.dot(gathered, ow[:, chunk], preferred_element_type=f32)

    copies = []
    for o in (2, 1, 3):
        peer = lax.rem(t + o, n_tp)
        osend[o] = out_columns(peer).astype(bf16)
        copies.append(remote(osend.at[o], orecv.at[o], o_sem.at[0, o], o_sem.at[1, o], e, peer))
    total = out_columns(t)
    for copy in copies:
        copy.wait_recv()
    for o in range(1, n_tp):
        total = total + orecv[o].astype(f32)
    pending += copies
    own_tokens = tokc[:, :, pl.ds(pl.multiple_of(t * cw, LANES), cw)].reshape(rows, cw)
    mix[t, e] = (own_tokens.astype(f32) + total).astype(bf16)
    arrivals, y_copies, d_copies = [], [], []
    for o in range(1, n_ep):
        peer = lax.rem(e + o, n_ep)
        arrivals.append(
            remote(mix.at[t, e], mix.at[t, e], g_sem.at[0, o], g_sem.at[1, o], peer, t)
        )
    for o in range(n_ep + 1):
        if o < n_ep:
            slot = mix.at[t, lax.rem(e + n_ep - o, n_ep)]
            if o > 0:
                arrivals[o - 1].wait_recv()
            y_copies.append(remote(slot, slot, gy_sem.at[0, o], gy_sem.at[1, o], e, ty))
            d_copies.append(remote(slot, slot, gd_sem.at[0, 0, o], gd_sem.at[1, 0, o], e, td))
        if o > 0:
            slot = mix.at[ty, lax.rem(e + n_ep - (o - 1), n_ep)]
            y_copies[o - 1].wait_recv()
            d_copies.append(
                remote(slot, slot, gd_sem.at[0, 1, o - 1], gd_sem.at[1, 1, o - 1], e, td)
            )
    for copy in d_copies:
        copy.wait_recv()
    pending += arrivals + y_copies + d_copies
    squares = jnp.zeros((rows, cw), jnp.float32)
    for j in range(n_tp):
        for i in range(n_ep):
            values = mix[j, i].astype(jnp.float32)
            squares = squares + values * values
    scale = lax.rsqrt(jnp.sum(squares, axis=-1, keepdims=True) / sec.shape[1] + EPS)
    gates = jnp.zeros((rows, cw), jnp.float32)
    for i in range(n_ep):
        for j in range(n_tp):
            at = (i * n_tp + j) * cw
            values = mix[j, i].astype(jnp.float32) * scale * mgain_ref[:, at : at + cw]
            values = values.astype(jnp.bfloat16)
            sec[:, at : at + cw] = values
            gates = gates + values.astype(jnp.float32) * vector_ref[:, at : at + cw]
    gate_value = jax.nn.sigmoid(jnp.sum(gates, axis=-1, keepdims=True))
    for load in loads[4:6]:
        load.wait()
    hid[t] = (
        jax.nn.silu(jnp.dot(sec[...], eg[...], preferred_element_type=f32))
        * jnp.dot(sec[...], eu[...], preferred_element_type=f32)
    ).astype(bf16)
    hidden_copies = []
    for o in (2, 1, 3):
        peer = lax.rem(t + o, n_tp)
        hidden_copies.append(
            remote(hid.at[t], hid.at[t], h_sem.at[0, o], h_sem.at[1, o], e, peer)
        )
    for load in loads[6:]:
        load.wait()
    dense_hidden = (
        jax.nn.silu(jnp.dot(sec[...], dg[...], preferred_element_type=f32))
        * jnp.dot(sec[...], du[...], preferred_element_type=f32)
    ).astype(bf16)
    dense = jnp.dot(dense_hidden, dd[...], preferred_element_type=f32)
    for copy in down_copies + hidden_copies:
        copy.wait_recv()
    pending += down_copies + hidden_copies
    expert_out = jnp.dot(hid[0], ed[0], preferred_element_type=f32)
    for j in range(1, n_tp):
        expert_out = expert_out + jnp.dot(hid[j], ed[j], preferred_element_type=f32)
    expert_out = expert_out.astype(bf16)
    lane = lax.broadcasted_iota(jnp.int32, (rows, LANES), 1)
    weight = jnp.sum(jnp.where(lane == e, aux, 0.0), axis=-1, keepdims=True)
    terms = weight * expert_out.astype(jnp.float32) + gate_value * dense
    csend[...] = terms.astype(jnp.bfloat16).reshape(n_ep, seqs, ocols)
    copies = []
    for o in range(1, n_ep):
        peer = lax.rem(e + o, n_ep)
        copies.append(
            remote(csend.at[peer], crecv.at[o], c_sem.at[0, o], c_sem.at[1, o], peer, t)
        )
    mine = pl.ds(pl.multiple_of(e * seqs, seqs), seqs)
    per_tp = n_ep // n_tp
    pieces = [mix[j, t * per_tp + k, mine, :] for k in range(per_tp) for j in range(n_tp)]
    total = jnp.concatenate(pieces, axis=1).astype(jnp.float32)
    total = total + csend[e].astype(jnp.float32)
    for o in range(1, n_ep):
        copies[o - 1].wait_recv()
        total = total + crecv[o].astype(jnp.float32)
    out_ref[...] = total.astype(jnp.bfloat16)
    for copy in pending + copies:
        copy.wait_send()


def fused_shards(
    tokens,
    norm_gain,
    query_weight,
    key_weight,
    value_weight,
    forget_weight,
    forget_bias,
    kv_cache,
    log_gates,
    lengths,
    out_weight,
    mix_gain,
    expert_gate,
    expert_up,
    expert_down,
    routes,
    route_weights,
    dense_gate,
    dense_up,
    dense_down,
    gate_vector,
):
    n_ep = lax.axis_size("ep")
    n_tp = lax.axis_size("tp")
    seqs, width = tokens.shape
    rows = n_ep * seqs
    cols = width // n_ep
    cw = cols // n_tp
    ocols = width // n_tp
    qc = query_weight.shape[1]
    hd = key_weight.shape[1]
    group = forget_weight.shape[1]
    count = kv_cache.shape[1]
    pw = qc + -(-(2 * hd + group) // LANES) * LANES
    vmem = pl.BlockSpec(memory_space=pltpu.VMEM)
    smem = pl.BlockSpec(memory_space=pltpu.SMEM)
    anywhere = pl.BlockSpec(memory_space=pl.ANY)
    dma = pltpu.SemaphoreType.DMA
    f32, bf16 = jnp.float32, jnp.bfloat16
    return pl.pallas_call(
        functools.partial(layer_kernel, n_ep, n_tp),
        out_shape=jax.ShapeDtypeStruct((seqs, ocols), bf16),
        in_specs=[vmem] * 10 + [smem] + [anywhere] * 10,
        out_specs=vmem,
        scratch_shapes=[
            pltpu.VMEM((n_ep, seqs, cols), bf16),
            pltpu.VMEM((seqs, LANES), f32),
            pltpu.VMEM((n_ep, seqs, LANES), f32),
            pltpu.VMEM((n_ep, seqs, pw), f32),
            pltpu.VMEM((n_ep, seqs, pw), f32),
            pltpu.VMEM(query_weight.shape, bf16),
            pltpu.VMEM((seqs, count, 2 * hd), bf16),
            pltpu.VMEM((seqs, group, count), f32),
            pltpu.VMEM((seqs, group, 2 * hd), f32),
            pltpu.VMEM((seqs, group, count), f32),
            pltpu.VMEM((seqs, group, count), bf16),
            pltpu.VMEM((seqs, group, 2 * hd), f32),
            pltpu.VMEM((seqs, qc), bf16),
            pltpu.VMEM((n_ep, seqs, qc), bf16),
            pltpu.VMEM(out_weight.shape, bf16),
            pltpu.VMEM(expert_gate.shape[1:], bf16),
            pltpu.VMEM(expert_up.shape[1:], bf16),
            pltpu.VMEM((n_tp, expert_down.shape[1], ocols), bf16),
            pltpu.VMEM(dense_gate.shape, bf16),
            pltpu.VMEM(dense_up.shape, bf16),
            pltpu.VMEM(dense_down.shape, bf16),
            pltpu.VMEM((n_tp, rows, cw), bf16),
            pltpu.VMEM((n_tp, rows, cw), bf16),
            pltpu.VMEM((n_tp, n_ep, rows, cw), bf16),
            pltpu.VMEM((rows, width), bf16),
            pltpu.VMEM((n_tp, rows, expert_gate.shape[2]), bf16),
            pltpu.VMEM((n_ep, seqs, ocols), bf16),
            pltpu.VMEM((n_ep, seqs, ocols), bf16),
            dma((10,)),
            dma((2, n_tp)),
            dma((2, n_ep)),
            dma((2, n_ep)),
            dma((2, n_ep)),
            dma((2, n_ep)),
            dma((2, n_tp)),
            dma((2, n_ep)),
            dma((2, n_ep)),
            dma((2, 2, n_ep)),
            dma((2, n_tp)),
            dma((2, n_ep)),
        ],
        compiler_params=pltpu.CompilerParams(
            collective_id=0, has_side_effects=True, vmem_limit_bytes=56 * 1024 * 1024
        ),
        name="layer",
    )(
        tokens,
        norm_gain.reshape(1, width),
        routes.T,
        route_weights.T,
        key_weight.T,
        value_weight.T,
        forget_weight.T,
        forget_bias.reshape(1, group),
        mix_gain.reshape(1, width),
        gate_vector.reshape(1, width),
        lengths,
        query_weight,
        kv_cache.reshape(seqs, count, 2 * hd),
        log_gates.transpose(0, 2, 1),
        out_weight,
        expert_gate,
        expert_up,
        expert_down,
        dense_gate,
        dense_up,
        dense_down,
    )


def layer(*arrays):
    tokens, routes = arrays[0], arrays[15]
    n_ep, n_tp = lax.axis_size("ep"), lax.axis_size("tp")
    seqs, width = tokens.shape
    capacity = seqs * routes.shape[1]
    fits = (
        n_tp == 4
        and n_ep % n_tp == 0
        and n_ep < LANES
        and n_ep * seqs <= 2 * capacity
        and width % (n_ep * n_tp * LANES) == 0
        and arrays[2].shape[1] % LANES == 0
        and arrays[7].shape[2] == 1
        and arrays[7].shape[3] == LANES
    )
    return (fused_shards if fits else shards)(*arrays)


def solution(mesh):
    return jax.shard_map(
        layer,
        mesh=mesh,
        in_specs=(
            P("ep", None),
            P(),
            P("ep", "tp"),
            P("ep", "tp"),
            P("ep", "tp"),
            P("ep", "tp"),
            P("tp"),
            P("ep", None, "tp", None),
            P("ep", None, "tp"),
            P("ep"),
            P("tp", "ep"),
            P(),
            P("ep", None, "tp"),
            P("ep", None, "tp"),
            P("ep", "tp", None),
            P("ep", None),
            P("ep", None),
            P(None, "ep"),
            P(None, "ep"),
            P("ep", "tp"),
            P(),
        ),
        out_specs=P("ep", "tp"),
        check_vma=False,
    )
```
